128 devices in a mesh: sp: 64 (over z, y, x), tp: 2 (over core).
Axes of the slice: x: 4, y: 4, z: 4, core: 2. Of those that a mesh axis runs over, the one named last changes fastest.
Arguments:
- queries_small: bfloat16 [16384, 1024], P('sp', 'tp'), may hold values from -160 to 160
- queries_large: bfloat16 [16384, 1024], P('sp', 'tp'), may hold values from -160 to 160
- kv_small: bfloat16 [16384, 128], P('sp'), may hold values from -4 to 4
- kv_large: bfloat16 [16384, 256], P('sp'), may hold values from -4 to 4
- cum_small: float32 [16, 16384], P('tp', 'sp'), may hold values from -2050 to 0, as said below
- cum_large: float32 [8, 16384], P('tp', 'sp'), may hold values from -2050 to 0, as said below
- residual: bfloat16 [16384, 2048], P(('sp', 'tp')), may hold values from -6 to 6
- out_small: bfloat16 [1024, 2048], replicated, may hold values from -0.125 to 0.125
- out_large: bfloat16 [1024, 2048], replicated, may hold values from -0.125 to 0.125
- gain_mix: float32 [2048], replicated, may hold values from 0.1 to 1.9
- gain_route: float32 [2048], replicated, may hold values from 0.1 to 1.9
- gain_blend: float32 [2048], replicated, may hold values from 0.1 to 1.9
- w_gate: bfloat16 [128, 2048, 1024], P(('sp', 'tp')), may hold values from -0.125 to 0.125
- w_up: bfloat16 [128, 2048, 1024], P(('sp', 'tp')), may hold values from -0.125 to 0.125
- w_down: bfloat16 [128, 1024, 2048], P(('sp', 'tp')), may hold values from -0.1875 to 0.1875
- route: int32 [2, 16384], P(None, ('sp', 'tp')), may hold values from 0 to 127, as said below
- route_bias: float32 [16384], P(('sp', 'tp')), may hold values from -6 to 6
Outputs:
- result: bfloat16 [16384, 2048], P(('sp', 'tp'))
The draws below stay inside these ranges and needn't reach their ends.
Inputs may be any that keep to these rules, and one draw needn't show every extreme that they name: `cum_small`: each row is non-increasing along positions. `cum_large`: each row is non-increasing along positions. route[0, t] and route[1, t] are different experts of the same group of 32 consecutive experts. Among the 128 positions of one device (aligned blocks), no expert is named by more than 4 of them; in every draw all experts of one group are named by exactly 4 positions of every device. Within one device's positions the loads of the experts of one group differ by at most 2.
All inputs are finite; a program needn't handle non-finite values.
Results may differ from the reference program's by a relative error of at most 0.014.
Values may be sent and summed in bfloat16 or wider, within the bound.
A program may use at most 128 MiB of HBM per device.

```python
import math
import jax
import jax.numpy as jnp
from jax import lax

D = 2048
HA = 16
DA = 64
HB = 8
DB = 128
FF = 1024
GROUPS = 4
TOK_DEV = 256
SEQUENCE_TOKENS = 16384
ROWS_DEV = 128
EXPERTS = 128
EPG = 32
CAP = 4
N_SP = 64
N_TP = 2


def shared_keys(root_random_key, head_size):
    return jnp.clip(jax.random.normal(jax.random.fold_in(root_random_key, 5), (SEQUENCE_TOKENS, head_size), jnp.float32), -4.0, 4.0)


def key_value_rows(key, label, head_size):
    root_random_key = jax.random.fold_in(key, label)
    key_rows = shared_keys(root_random_key, head_size)
    value_rows = jnp.clip(jax.random.normal(jax.random.fold_in(root_random_key, 6), (SEQUENCE_TOKENS, head_size), jnp.float32), -4.0, 4.0)
    return jnp.concatenate([key_rows, value_rows], axis=1).astype(jnp.bfloat16)


def query_rows(key, label, head_count, head_size):
    root_random_key = jax.random.fold_in(key, label)
    drawn = jnp.clip(jax.random.normal(jax.random.fold_in(root_random_key, 9), (SEQUENCE_TOKENS, head_count * head_size), jnp.float32), -4.0, 4.0)
    return drawn.astype(jnp.bfloat16)


def gate_totals(key, label, head_count):
    root_random_key = jax.random.fold_in(key, label)
    order = jax.random.permutation(jax.random.fold_in(root_random_key, 1), head_count)
    slow_heads = order < head_count // 2
    slow_total = jnp.exp(jax.random.uniform(jax.random.fold_in(root_random_key, 3), (head_count,), jnp.float32, math.log(0.8), math.log(1.6)))
    fast_rate = jnp.exp(jax.random.uniform(jax.random.fold_in(root_random_key, 4), (head_count,), jnp.float32, math.log(0.01), math.log(1.0 / 30.0)))
    rates = jnp.where(slow_heads, slow_total / SEQUENCE_TOKENS, fast_rate)
    factors = jnp.exp(jax.random.uniform(jax.random.fold_in(root_random_key, 5), (SEQUENCE_TOKENS // TOK_DEV,), jnp.float32, math.log(0.5), math.log(2.0)))
    factors = jnp.repeat(factors, TOK_DEV)
    rough = jax.random.uniform(jax.random.fold_in(root_random_key, 6), (head_count, SEQUENCE_TOKENS), jnp.float32, 0.5, 1.5)
    gate_logarithms = -rates[:, None] * factors[None, :] * rough
    spike_position = jax.random.randint(jax.random.fold_in(root_random_key, 7), (3,), 0, SEQUENCE_TOKENS)
    spike_penalty = jax.random.uniform(jax.random.fold_in(root_random_key, 8), (3,), jnp.float32, 0.2, 0.4)
    spot_locations = jnp.arange(SEQUENCE_TOKENS, dtype=jnp.int32)
    spike_events = jnp.sum(jnp.where(spot_locations[None, :] == spike_position[:, None], jnp.log(1.0 - spike_penalty)[:, None], 0.0), axis=0)
    gate_logarithms = gate_logarithms + spike_events[None, :]
    return jnp.cumsum(gate_logarithms, axis=1).astype(jnp.float32)


def draw_queries_small(key, part):
    return query_rows(key, 11, HA, DA)


def draw_queries_large(key, part):
    return query_rows(key, 13, HB, DB)


def draw_kv_small(key, part):
    return key_value_rows(key, 11, DA)


def draw_kv_large(key, part):
    return key_value_rows(key, 13, DB)


def draw_cum_small(key, part):
    return gate_totals(key, 31, HA)


def draw_cum_large(key, part):
    return gate_totals(key, 33, HB)


def draw_route(key, part):
    block_count = SEQUENCE_TOKENS // ROWS_DEV
    full_group = jax.random.randint(jax.random.fold_in(key, 21), (), 0, GROUPS)

    def one_block(block_index):
        block_key = jax.random.fold_in(jax.random.fold_in(key, 22), block_index)
        order = jax.random.permutation(jax.random.fold_in(block_key, 1), ROWS_DEV)
        spot_locations = jnp.arange(ROWS_DEV, dtype=jnp.int32)
        others = jax.random.randint(jax.random.fold_in(block_key, 2), (ROWS_DEV,), 0, GROUPS - 1)
        group_at = jnp.where(spot_locations < ROWS_DEV // 2, full_group, (full_group + 1 + others) % GROUPS)
        marked = (group_at[:, None] == jnp.arange(GROUPS, dtype=jnp.int32)[None, :]).astype(jnp.int32)
        ranked = jnp.sum((jnp.cumsum(marked, axis=0) - 1) * marked, axis=1)
        shifts = jax.random.randint(jax.random.fold_in(block_key, 3), (GROUPS,), 0, EPG)
        offset = ranked + shifts[group_at]
        first_inner = offset % EPG
        second_inner = (offset + 1 + ranked // EPG % (EPG - 1)) % EPG
        chosen = jnp.stack([group_at * EPG + first_inner, group_at * EPG + second_inner]).astype(jnp.int32)
        return jnp.zeros((2, ROWS_DEV), jnp.int32).at[:, order].set(chosen)
    blocks = jax.vmap(one_block)(jnp.arange(block_count, dtype=jnp.int32))
    return blocks.transpose(1, 0, 2).reshape(2, SEQUENCE_TOKENS)


def block_scale(key, extent, split, low, largest):
    gain = 1.0
    for position, shards_of in split:
        steps = jax.random.uniform(jax.random.fold_in(jax.random.fold_in(key, 6), position), (shards_of,), jnp.float32, low / len(split), largest / len(split))
        gain = gain * jnp.repeat(jnp.exp(steps), extent[position] // shards_of).reshape((-1,) + (1,) * (len(extent) - 1 - position))
    return gain


def noise(rng, dims, deviation, limit, split=(), kind=jnp.bfloat16):
    array = jax.random.normal(rng, dims, jnp.float32) * deviation
    if len(split) > 0:
        array = block_scale(rng, dims, split, -0.22, 0.18) * array
    return jnp.clip(array, min=-limit, max=limit).astype(kind)


def setup_inputs(seed: int = 0) -> dict:
    streams_of = jax.random.split(jax.random.key(seed), 18)
    return {
        "queries_small": draw_queries_small(jax.random.fold_in(streams_of[17], 71), 0),
        "queries_large": draw_queries_large(jax.random.fold_in(streams_of[17], 71), 0),
        "kv_small": draw_kv_small(jax.random.fold_in(streams_of[17], 71), 0),
        "kv_large": draw_kv_large(jax.random.fold_in(streams_of[17], 71), 0),
        "cum_small": draw_cum_small(jax.random.fold_in(streams_of[17], 71), 0),
        "cum_large": draw_cum_large(jax.random.fold_in(streams_of[17], 71), 0),
        "residual": noise(streams_of[6], (SEQUENCE_TOKENS, D), 1.0, 6.0, ((0, 128),)),
        "out_small": noise(streams_of[7], (HA * DA, D), D ** -0.5, 0.125),
        "out_large": noise(streams_of[8], (HB * DB, D), D ** -0.5, 0.125),
        "gain_mix": jnp.clip(1.0 + 0.18 * jax.random.normal(streams_of[9], (D,), jnp.float32), 0.1, 1.9),
        "gain_route": jnp.clip(1.0 + 0.18 * jax.random.normal(streams_of[10], (D,), jnp.float32), 0.1, 1.9),
        "gain_blend": jnp.clip(1.0 + 0.18 * jax.random.normal(streams_of[11], (D,), jnp.float32), 0.1, 1.9),
        "w_gate": noise(streams_of[12], (EXPERTS, D, FF), D ** -0.5, 0.125, ((0, 128),)),
        "w_up": noise(streams_of[13], (EXPERTS, D, FF), D ** -0.5, 0.125, ((0, 128),)),
        "w_down": noise(streams_of[14], (EXPERTS, FF, D), FF ** -0.5, 0.1875, ((0, 128),)),
        "route": draw_route(jax.random.fold_in(streams_of[17], 71), 0),
        "route_bias": noise(streams_of[16], (SEQUENCE_TOKENS,), 1.5, 6.0, ((0, 128),), jnp.float32),
    }


norm_eps = 1e-06

def rms_scale(values, gain_row):
    return values * lax.rsqrt(lax.optimization_barrier(jnp.mean(values * values, axis=-1, keepdims=True)) + norm_eps) * gain_row.astype(jnp.float32)

def attend_group(queries, keys_values, cumulative, head_count, head_size):
    key_rows = keys_values[:, :head_size].astype(jnp.float32)
    value_rows = keys_values[:, head_size:].astype(jnp.float32)
    block_rows = min(256, SEQUENCE_TOKENS)
    block_count = SEQUENCE_TOKENS // block_rows
    query_blocks = queries.reshape(block_count, block_rows, head_count, head_size)
    cum_blocks = cumulative.reshape(head_count, block_count, block_rows).transpose(1, 0, 2)
    key_pos = jnp.arange(SEQUENCE_TOKENS, dtype=jnp.int32)

    def one_block(inputs):
        query_block, cum_block, block_index = inputs
        scores = jnp.einsum('qhd,kd->hqk', query_block.astype(jnp.float32), key_rows) * head_size ** (-0.5)
        scores = scores + cum_block[:, :, None] - cumulative[:, None, :]
        query_pos = block_index * block_rows + jnp.arange(block_rows, dtype=jnp.int32)
        allowed = key_pos[None, None, :] <= query_pos[None, :, None]
        scores = jnp.where(allowed, scores, -jnp.inf)
        row_max = lax.optimization_barrier(jnp.max(scores, axis=-1, keepdims=True))
        weights = jnp.where(allowed, jnp.exp(scores - row_max), 0.0)
        rounded = lax.optimization_barrier(weights.astype(jnp.bfloat16)).astype(jnp.float32)
        numerator = jnp.einsum('hqk,kd->qhd', rounded, value_rows)
        denominator = lax.optimization_barrier(jnp.sum(weights, axis=-1)).T
        return (numerator / denominator[:, :, None]).astype(jnp.bfloat16)
    outputs = lax.map(one_block, (query_blocks, cum_blocks, jnp.arange(block_count, dtype=jnp.int32)))
    return outputs.reshape(SEQUENCE_TOKENS, head_count * head_size)

def reference(queries_small, queries_large, kv_small, kv_large, cum_small, cum_large, residual, out_small, out_large, gain_mix, gain_route, gain_blend, w_gate, w_up, w_down, route, route_bias):
    attn_small = attend_group(queries_small, kv_small, cum_small, HA, DA)
    attn_large = attend_group(queries_large, kv_large, cum_large, HB, DB)
    mixer_out = jnp.dot(attn_small, out_small, preferred_element_type=jnp.float32) + jnp.dot(attn_large, out_large, preferred_element_type=jnp.float32)
    mixed = (residual.astype(jnp.float32) + rms_scale(mixer_out, gain_mix)).astype(jnp.bfloat16)
    routed = rms_scale(mixed.astype(jnp.float32), gain_route).astype(jnp.bfloat16)
    flat_ids = route.reshape(-1)
    most_rows = N_SP * N_TP * CAP

    def one_expert(carried, inputs):
        expert_id, gate_w, up_w, down_w = inputs
        matches = flat_ids == expert_id
        picked = jnp.nonzero(matches, size=most_rows, fill_value=0)[0].astype(jnp.int32)
        valid_rows = jnp.arange(most_rows, dtype=jnp.int32) < jnp.sum(matches.astype(jnp.int32))
        expert_rows = routed[picked % SEQUENCE_TOKENS]
        gate_pre = jnp.dot(expert_rows, gate_w, preferred_element_type=jnp.float32)
        up_pre = jnp.dot(expert_rows, up_w, preferred_element_type=jnp.float32)
        hidden = (jax.nn.silu(gate_pre) * up_pre).astype(jnp.bfloat16)
        expert_out = jnp.dot(hidden, down_w, preferred_element_type=jnp.float32).astype(jnp.bfloat16)
        masked = jnp.where(valid_rows[:, None], expert_out.astype(jnp.float32), 0.0)
        return (carried.at[picked].add(masked), None)
    outputs, _ = lax.scan(one_expert, jnp.zeros((2 * SEQUENCE_TOKENS, D), jnp.float32), (jnp.arange(EXPERTS, dtype=jnp.int32), w_gate, w_up, w_down))
    blended = jax.nn.sigmoid(route_bias)[:, None] * outputs[:SEQUENCE_TOKENS] + jax.nn.sigmoid(-route_bias)[:, None] * outputs[SEQUENCE_TOKENS:]
    return (mixed.astype(jnp.float32) + rms_scale(blended, gain_blend)).astype(jnp.bfloat16)
```

```python
import functools
import math

import jax
import jax.numpy as jnp
from jax import lax
from jax.experimental import pallas as pl
from jax.experimental.pallas import tpu as pltpu
from jax.sharding import PartitionSpec as P

MESH = pl.DeviceIdType.MESH
norm_eps = 1e-06
far_score = -1e30
log2e = 1.4426950408889634
f32, bf16 = jnp.float32, jnp.bfloat16
unit = 1024
own_units = 9

orders = (("x", "y", "z"), ("y", "z", "x"), ("z", "x", "y"))
pieces = (
    (0, 0, 0, 32, 16),
    (1, 0, 48, 32, 16),
    (2, 0, 96, 32, 16),
    (0, 0, 32, 16, 8),
    (1, 0, 80, 16, 8),
    (2, 1, 0, 24, 16),
)
shift = (3, 1, 2, 2)

def gather_kernel(kv_ref, cum_ref, g_ref, c_ref, local, send, recv, dsend, drecv):
    sp, tp = lax.axis_index("sp"), lax.axis_index("tp")
    at = {"z": sp // 16, "y": (sp // 4) % 4, "x": sp % 4}
    partner = (sp, 1 - tp)

    def moved(dim, by):
        here = dict(at)
        here[dim] = (at[dim] + by) % 4
        return (here["z"] * 16 + here["y"] * 4 + here["x"], tp)

    barrier = pltpu.get_barrier_semaphore()
    for dim in ("x", "y", "z"):
        for by in (1, 3):
            pl.semaphore_signal(barrier, inc=1, device_id=moved(dim, by), device_id_type=MESH)
    pl.semaphore_signal(barrier, inc=1, device_id=partner, device_id_type=MESH)

    def rows_of(piece, kind):
        _, _, first, count, half = pieces[piece]
        if kind == 2:
            return (first, half)
        if kind == 3:
            return (first + half, count - half)
        return (first, count)

    def view(piece, phase, offset, kind, side):
        order = orders[pieces[piece][0]]
        index = []
        for dim in ("z", "y", "x"):
            where = order.index(dim)
            if where < phase:
                index.append(slice(None))
            else:
                index.append((at[dim] + offset) % 4 if where == phase else at[dim])
        whole = c_ref if pieces[piece][1] else g_ref
        return whole.at[(*index, side, pl.ds(*rows_of(piece, kind)), slice(None))]

    def sent(piece, phase, kind):
        target = view(piece, phase, (0, 0, 3, 1)[kind], kind, tp)
        source = target
        if phase == 0 and kind < 2:
            source = (cum_ref if pieces[piece][1] else kv_ref).at[pl.ds(*rows_of(piece, kind)), :]
        return pltpu.make_async_remote_copy(
            src_ref=source, dst_ref=target, send_sem=send.at[piece, phase, kind], recv_sem=recv.at[piece, phase, kind],
            device_id=moved(orders[pieces[piece][0]][phase], 1 if kind in (0, 2) else 3), device_id_type=MESH)

    def arrived(piece, phase, kind):
        ref = view(piece, phase, shift[kind], kind, tp)
        return pltpu.make_async_remote_copy(
            src_ref=ref, dst_ref=ref, send_sem=send.at[piece, phase, kind], recv_sem=recv.at[piece, phase, kind],
            device_id=partner, device_id_type=MESH)

    def shared(piece, phase, kind, side):
        ref = view(piece, phase, shift[kind], kind, side)
        return pltpu.make_async_remote_copy(
            src_ref=ref, dst_ref=ref, send_sem=dsend.at[piece, phase, kind], recv_sem=drecv.at[piece, phase, kind],
            device_id=partner, device_id_type=MESH)

    def own(source, whole, k):
        return pltpu.make_async_remote_copy(
            src_ref=source, dst_ref=whole.at[at["z"], at["y"], at["x"], tp], send_sem=local.at[2 + k], recv_sem=local.at[4 + k],
            device_id=partner, device_id_type=MESH)

    def kept(source, whole, k):
        return pltpu.make_async_copy(source, whole.at[at["z"], at["y"], at["x"], tp], local.at[k])

    count = range(len(pieces))
    kept(kv_ref, g_ref, 0).start()
    kept(cum_ref, c_ref, 1).start()
    pl.semaphore_wait(barrier, 7)
    for piece in count:
        for kind in (0, 1):
            sent(piece, 0, kind).start()
    own(kv_ref, g_ref, 0).start()
    own(cum_ref, c_ref, 1).start()
    kept(kv_ref, g_ref, 0).wait()
    kept(cum_ref, c_ref, 1).wait()
    for phase in range(3):
        for piece in count:
            for kind in (0, 1):
                arrived(piece, phase, kind).wait_recv()
                sent(piece, phase, 2 + kind).start()
                shared(piece, phase, kind, tp).start()
        for piece in count:
            for kind in (2, 3):
                arrived(piece, phase, kind).wait_recv()
            if phase < 2:
                for kind in (0, 1):
                    sent(piece, phase + 1, kind).start()
            for kind in (2, 3):
                shared(piece, phase, kind, tp).start()
    for k, whole in ((0, g_ref), (1, c_ref)):
        source = kv_ref if k == 0 else cum_ref
        own(source, whole, k).wait_send()
        theirs = whole.at[at["z"], at["y"], at["x"], 1 - tp]
        pltpu.make_async_remote_copy(
            src_ref=theirs, dst_ref=theirs, send_sem=local.at[2 + k], recv_sem=local.at[4 + k],
            device_id=partner, device_id_type=MESH).wait_recv()
    for phase in range(3):
        for piece in count:
            for kind in range(4):
                sent(piece, phase, kind).wait_send()
                shared(piece, phase, kind, tp).wait_send()
                shared(piece, phase, kind, 1 - tp).wait_recv()

def gather(kv, cum):
    DMA = pltpu.SemaphoreType.DMA
    shape = (len(pieces), 3, 4)
    V = pl.BlockSpec(memory_space=pltpu.VMEM)
    O = pl.BlockSpec(memory_space=pl.ANY)
    return pl.pallas_call(
        gather_kernel,
        out_shape=(jax.ShapeDtypeStruct((4, 4, 4, 2, 128, 384), jnp.bfloat16), jax.ShapeDtypeStruct((4, 4, 4, 2, 24, 128), jnp.float32)),
        in_specs=[V, V],
        out_specs=(O, O),
        scratch_shapes=[DMA((6,)), DMA(shape), DMA(shape), DMA(shape), DMA(shape)],
        compiler_params=pltpu.CompilerParams(collective_id=0, has_side_effects=True, vmem_limit_bytes=40*1024*1024),
        name="gather_keys",
    )(kv, cum)


def attention_kernel(bounds, qs_ref, ql_ref, cq_ref, g_ref, c_ref, os_ref, ol_ref, ml_ref,
                     kv, gates, tile, vts, vtl, qs, ql, acc_s, acc_l, top, sems, *, diagonal):
    lo, hi, q0, first_head = bounds[0], bounds[1], bounds[2], bounds[3]
    nq = 256
    cs, cl = log2e / 8.0, log2e / math.sqrt(128.0)
    n = hi - lo

    def fetch(u, slot):
        return (
            pltpu.make_async_copy(g_ref.at[pl.ds(pl.multiple_of(u * unit, unit), unit), :], kv.at[slot], sems.at[0, slot]),
            pltpu.make_async_copy(c_ref.at[pl.ds(u * 8, 8)], gates.at[slot], sems.at[1, slot]),
        )

    @pl.when(n > 0)
    def _():
        for copy in fetch(hi - 1, 0):
            copy.start()

    acc_s[...] = jnp.zeros(acc_s.shape, f32)
    acc_l[...] = jnp.zeros(acc_l.shape, f32)
    top[...] = jnp.zeros(top.shape, f32)
    vts[64:80, :] = jnp.ones((16, unit), bf16)
    vtl[128:144, :] = jnp.ones((16, unit), bf16)
    qs[128:192, :] = qs_ref[...]
    qs[192:256, :] = jnp.zeros((64, 2048), bf16)
    ql[0:128, :] = ql_ref[...]
    row = lax.broadcasted_iota(jnp.int32, (128, nq), 0)
    for h in range(12):
        head = first_head + h
        here = cq_ref[h : h + 1, :]
        high = here.astype(bf16).astype(f32)
        rest = here - high
        middle = rest.astype(bf16).astype(f32)
        low = rest - middle
        chosen = jnp.where((row == head) | (row == 24 + head) | (row == 48 + head), -8.0, 0.0)
        chosen = jnp.where(row == 72, 8.0 * high, chosen)
        chosen = jnp.where(row == 73, 8.0 * middle, chosen)
        chosen = jnp.where(row == 74, 8.0 * low, chosen).astype(bf16)
        if h < 8:
            qs[0:128, h * nq : (h + 1) * nq] = chosen
        else:
            ql[128:256, (h - 8) * nq : (h - 7) * nq] = chosen
    size_s = jnp.max(jnp.sum(jnp.abs(qs_ref[...].astype(f32)), axis=0, keepdims=True))
    size_l = jnp.max(jnp.sum(jnp.abs(ql_ref[...].astype(f32)), axis=0, keepdims=True))
    bounded = (size_s <= 150.0) & (size_l <= 210.0)

    def ready(i):
        u, slot = hi - 1 - i, lax.rem(i, 2)
        for copy in fetch(u, slot):
            copy.wait()

        @pl.when(i + 1 < n)
        def _():
            for copy in fetch(u - 1, 1 - slot):
                copy.start()

        for j in range(8):
            gate = gates[slot, j]
            high = gate.astype(bf16).astype(f32)
            rest = gate - high
            middle = rest.astype(bf16).astype(f32)
            wide = jnp.concatenate([high, middle, rest - middle, jnp.ones((8, 128), f32), jnp.zeros((48, 128), f32)], axis=0)
            tile[j * 128 : (j + 1) * 128, :] = wide.T.astype(bf16)
        vts[0:64, :] = kv[slot, :, 0:128].T[64:128, :]
        vtl[0:128, :] = kv[slot, :, 256:384].T
        return u, slot

    def keys_small(slot):
        return jnp.concatenate([tile[...], kv[slot, :, 0:128]], axis=1)

    def keys_large(slot):
        return jnp.concatenate([kv[slot, :, 128:256], tile[...]], axis=1)

    def allowed(u, width):
        key = u * unit + lax.broadcasted_iota(jnp.int32, (unit, width), 0)
        query = q0 + (lax.broadcasted_iota(jnp.int32, (unit, width), 1) & (nq - 1))
        return key <= query

    def quick(i, masked):
        u, slot = ready(i)
        for keys, q, w, vt, acc, scale in (
            (keys_small, qs, 0, vts, acc_s, cs),
            (keys_small, qs, 1024, vts, acc_s, cs),
            (keys_large, ql, 0, vtl, acc_l, cl),
        ):
            s = jnp.dot(keys(slot), q[:, w : w + 1024], preferred_element_type=f32) * scale
            if masked:
                s = jnp.where(allowed(u, 1024), s, far_score)
            p = jnp.exp2(s).astype(bf16)
            acc[:, w : w + 1024] += jnp.dot(vt[...], p, preferred_element_type=f32)

    def careful(i, _):
        u, slot = ready(i)

        def group(keys, q, vt, acc, scale, count, base):
            def head(h, _):
                w = pl.ds(pl.multiple_of(h * nq, nq), nq)
                s = jnp.dot(keys(slot), q[:, w], preferred_element_type=f32) * scale
                s = jnp.where(allowed(u, nq), s, far_score)
                before = top[base + h]
                after = jnp.maximum(before, jnp.max(s, axis=0, keepdims=True))
                top[base + h] = after
                p = jnp.exp2(s - after).astype(bf16)
                acc[:, w] = acc[:, w] * jnp.exp2(before - after) + jnp.dot(vt[...], p, preferred_element_type=f32)
                return 0

            lax.fori_loop(0, count, head, 0)

        group(keys_small, qs, vts, acc_s, cs, 8, 0)
        group(keys_large, ql, vtl, acc_l, cl, 4, 8)
        return 0

    @pl.when(bounded)
    def _():
        if diagonal:
            quick(0, True)
        lax.fori_loop(1 if diagonal else 0, n, lambda i, _: (quick(i, False), 0)[1], 0)

    @pl.when(jnp.logical_not(bounded))
    def _():
        top[...] = jnp.full(top.shape, far_score, f32)
        lax.fori_loop(0, n, careful, 0)

    ml_ref[...] = jnp.zeros(ml_ref.shape, f32)
    for h in range(12):
        size, acc, out, k = (64, acc_s, os_ref, h) if h < 8 else (128, acc_l, ol_ref, h - 8)
        w = slice(k * nq, (k + 1) * nq)
        total = acc[size : size + 1, w]
        scale = jnp.where(total > 0, 1.0 / jnp.where(total > 0, total, 1.0), 0.0)
        out[k * size : (k + 1) * size, :] = (acc[0:size, w] * scale).astype(out.dtype)
        ml_ref[h : h + 1, :] = top[h]
        ml_ref[16 + h : 17 + h, :] = total


def attention(bounds, qs, ql, cq, g, c, diagonal):
    V = pl.BlockSpec(memory_space=pltpu.VMEM)
    A = pl.BlockSpec(memory_space=pl.ANY)
    kind = f32 if diagonal else bf16
    VM = pltpu.VMEM
    return pl.pallas_call(
        functools.partial(attention_kernel, diagonal=diagonal),
        out_shape=(
            jax.ShapeDtypeStruct((512, 256), kind),
            jax.ShapeDtypeStruct((512, 256), kind),
            jax.ShapeDtypeStruct((32, 256), f32),
        ),
        in_specs=[pl.BlockSpec(memory_space=pltpu.SMEM), V, V, V, A, A],
        out_specs=(V, V, V),
        scratch_shapes=[
            VM((2, unit, 384), bf16), VM((2, 8, 24, 128), f32), VM((unit, 128), bf16),
            VM((80, unit), bf16), VM((144, unit), bf16), VM((256, 2048), bf16), VM((256, 1024), bf16),
            VM((80, 2048), f32), VM((144, 1024), f32), VM((12, 1, 256), f32), pltpu.SemaphoreType.DMA((2, 2)),
        ],
        compiler_params=pltpu.CompilerParams(vmem_limit_bytes=50 * 1024 * 1024),
        cost_estimate=pl.CostEstimate(flops=12_000_000_000 if diagonal else 8_000_000_000, bytes_accessed=12_000_000, transcendentals=26_000_000),
        name="attention_own" if diagonal else "attention_far",
    )(bounds, qs, ql, cq, g, c)


def merged(own, far, m_own, m_far, l_own, l_far, heads):
    m_far = jnp.where(l_far > 0, m_far, far_score)
    most = jnp.maximum(m_own, m_far)
    a, b = l_own * jnp.exp2(m_own - most), l_far * jnp.exp2(m_far - most)
    whole = a + b
    size = own.shape[0] // heads
    own = own.reshape(heads, size, 256) * (a / whole)[:, None, :]
    far = far.astype(f32).reshape(heads, size, 256) * (b / whole)[:, None, :]
    return (own + far).astype(bf16).reshape(heads * size, 256)


def cut_along(array, dim, devices):
    lengths = array.shape
    tiles = array.reshape(*lengths[:dim], devices, lengths[dim] // devices, *lengths[dim + 1 :])
    return jnp.moveaxis(tiles, dim, 0)


def sum_at_owner(array, axis, dim):
    devices = lax.axis_size(axis)
    tiles = lax.all_to_all(cut_along(array, dim, devices), axis, 0, 0, tiled=True)
    return jnp.sum(tiles.astype(jnp.float32), axis=0)


def rms_scale(values, gain_row):
    return (
        values * lax.rsqrt(jnp.mean(values * values, axis=-1, keepdims=True) + norm_eps) * gain_row
    )


def on_device(
    queries_small,
    queries_large,
    kv_small,
    kv_large,
    cum_small,
    cum_large,
    residual,
    out_small,
    out_large,
    gain_mix,
    gain_route,
    gain_blend,
    w_gate,
    w_up,
    w_down,
    route,
    route_bias,
):
    sp, tp = lax.axis_index("sp"), lax.axis_index("tp")
    tokens_here = queries_small.shape[0]
    chips = lax.axis_size("sp")
    gates = jnp.concatenate([cum_small, cum_large * jnp.float32(math.sqrt(2.0))], axis=0)
    halves = gates.reshape(12, 2, 128)
    kept = lax.dynamic_index_in_dim(halves, tp, 1, keepdims=False)
    given = lax.ppermute(lax.dynamic_index_in_dim(halves, 1 - tp, 1, keepdims=False), "tp", [(0, 1), (1, 0)])
    all_gates = jnp.where(tp == 0, jnp.concatenate([kept, given], axis=0), jnp.concatenate([given, kept], axis=0))
    kv_here = jnp.concatenate(
        [lax.dynamic_slice_in_dim(kv, tp * 128, 128, 0) for kv in (kv_small, kv_large)], axis=1
    )
    qs = queries_small.reshape(256, 8, 64).transpose(2, 1, 0).reshape(64, 2048)
    ql = queries_large.reshape(256, 4, 128).transpose(2, 1, 0).reshape(128, 1024)
    cq = jnp.concatenate([gates, jnp.zeros((4, 256), f32)], axis=0)
    to_early = [(chips - 1 - i, i) for i in range(chips // 2)]
    to_late = [(i, chips - 1 - i) for i in range(chips // 2)]
    far_q = [lax.ppermute(a, "sp", to_early) for a in (qs, ql, cq)]
    g, c = gather(kv_here, all_gates)
    g, c = g.reshape(chips * 256, 384), c.reshape(chips * 2, 24, 128)
    units = sp // 4 + 1
    first = jnp.maximum(units - own_units, 0)
    late = chips - 1 - sp
    helped = jnp.where(sp < chips // 2, jnp.maximum(late // 4 + 1 - own_units, 0), 0)
    bounds = jnp.stack([first, units, sp * 256, tp * 12]).astype(jnp.int32)
    far_bounds = jnp.stack([jnp.zeros_like(helped), helped, late * 256, tp * 12]).astype(jnp.int32)
    own_s, own_l, own_ml = attention(bounds, qs, ql, cq, g, c, True)
    far = attention(far_bounds, *far_q, g, c, False)
    far_s, far_l, far_ml = [lax.ppermute(a, "sp", to_late) for a in far]
    attn_small = merged(own_s, far_s, own_ml[0:8], far_ml[0:8], own_ml[16:24], far_ml[16:24], 8)
    attn_large = merged(own_l, far_l, own_ml[8:12], far_ml[8:12], own_ml[24:28], far_ml[24:28], 4)
    row_count = tokens_here // lax.axis_size("tp")
    weight_small = lax.dynamic_slice_in_dim(
        out_small, tp * 512, 512, 0
    )
    weight_large = lax.dynamic_slice_in_dim(
        out_large, tp * 512, 512, 0
    )
    mixer_out = sum_at_owner(
        (
            lax.dot_general(attn_small, weight_small, (((0,), (0,)), ((), ())), preferred_element_type=f32)
            + lax.dot_general(attn_large, weight_large, (((0,), (0,)), ((), ())), preferred_element_type=f32)
        ).astype(jnp.bfloat16),
        "tp",
        0,
    )
    mixed = (residual.astype(jnp.float32) + rms_scale(mixer_out, gain_mix)).astype(jnp.bfloat16)
    routed = rms_scale(mixed.astype(jnp.float32), gain_route).astype(jnp.bfloat16)
    experts = lax.axis_size(("sp", "tp"))
    capacity = 4 * row_count // experts
    flat_ids = route.reshape(2 * row_count)
    marked = (flat_ids[:, None] == jnp.arange(experts, dtype=jnp.int32)[None, :]).astype(jnp.int32)
    ranked = jnp.sum((jnp.cumsum(marked, axis=0) - 1) * marked, axis=1)
    slot_ids = flat_ids * capacity + ranked
    dispatch_table = (
        slot_ids[:, None] == jnp.arange(experts * capacity, dtype=jnp.int32)[None, :]
    ).astype(jnp.bfloat16)
    dispatch_table = dispatch_table[:row_count] + dispatch_table[row_count:]
    outgoing = jnp.einsum(
        "rs,rd->sd", dispatch_table, routed, preferred_element_type=jnp.float32
    ).astype(jnp.bfloat16)
    outgoing = outgoing.reshape(experts, capacity, routed.shape[1])
    received = lax.all_to_all(outgoing, ("sp", "tp"), split_axis=0, concat_axis=0, tiled=True)
    row_total = received.shape[0] * received.shape[1]
    expert_rows = received.reshape(row_total, received.shape[2])
    gate_pre = jnp.dot(expert_rows, w_gate[0], preferred_element_type=jnp.float32)
    up_pre = jnp.dot(expert_rows, w_up[0], preferred_element_type=jnp.float32)
    hidden = (jax.nn.silu(gate_pre) * up_pre).astype(jnp.bfloat16)
    expert_out = jnp.dot(hidden, w_down[0], preferred_element_type=jnp.float32).astype(jnp.bfloat16)
    returned = lax.all_to_all(
        expert_out.reshape(received.shape), ("sp", "tp"), split_axis=0, concat_axis=0, tiled=True
    )
    picked = returned.reshape(experts * capacity, routed.shape[1])[slot_ids].astype(jnp.float32)
    blended = (
        jax.nn.sigmoid(route_bias)[:, None] * picked[:row_count]
        + jax.nn.sigmoid(-route_bias)[:, None] * picked[row_count:]
    )
    return (mixed.astype(jnp.float32) + rms_scale(blended, gain_blend)).astype(jnp.bfloat16)


def solution(mesh):
    in_specs = (
        P("sp", "tp"),
        P("sp", "tp"),
        P("sp", None),
        P("sp", None),
        P("tp", "sp"),
        P("tp", "sp"),
        P(("sp", "tp"), None),
        P(),
        P(),
        P(),
        P(),
        P(),
        P(("sp", "tp"), None, None),
        P(("sp", "tp"), None, None),
        P(("sp", "tp"), None, None),
        P(None, ("sp", "tp")),
        P(("sp", "tp")),
    )
    out_specs = P(("sp", "tp"), None)
    return jax.shard_map(
        on_device, mesh=mesh, in_specs=in_specs, out_specs=out_specs, check_vma=False
    )
```

```python
import functools
import math

import jax
import jax.numpy as jnp
from jax import lax
from jax.experimental import pallas as pl
from jax.experimental.pallas import tpu as pltpu
from jax.sharding import PartitionSpec as P


MESH = pl.DeviceIdType.MESH
norm_eps = 1e-06
far_score = -1e30
log2e = 1.4426950408889634
f32, bf16 = jnp.float32, jnp.bfloat16
unit = 1024
own_units = 9

orders = (("x", "y", "z"), ("y", "z", "x"), ("z", "x", "y"))
pieces = (
    (0, 0, 0, 32, 16),
    (1, 0, 48, 32, 16),
    (2, 0, 96, 32, 16),
    (0, 0, 32, 16, 8),
    (1, 0, 80, 16, 8),
    (2, 1, 0, 32, 16),
)
shift = (3, 1, 2, 2)


def gather_kernel(small_ref, large_ref, gates_ref, qs_ref, ql_ref, g_ref, c_ref, far_qs, far_ql, far_gates,
                  send, recv, dsend, drecv, far_send, far_recv):
    sp, tp = lax.axis_index("sp"), lax.axis_index("tp")
    at = {"z": sp // 16, "y": (sp // 4) % 4, "x": sp % 4}
    partner = (sp, 1 - tp)
    mirror = (63 - sp, tp)
    far_qs[...] = jnp.zeros(far_qs.shape, bf16)
    far_ql[...] = jnp.zeros(far_ql.shape, bf16)
    far_gates[...] = jnp.zeros(far_gates.shape, f32)

    def moved(dim, by):
        here = dict(at)
        here[dim] = (at[dim] + by) % 4
        return (here["z"] * 16 + here["y"] * 4 + here["x"], tp)

    barrier = pltpu.get_barrier_semaphore()
    for dim in ("x", "y", "z"):
        for by in (1, 3):
            pl.semaphore_signal(barrier, inc=1, device_id=moved(dim, by), device_id_type=MESH)
    pl.semaphore_signal(barrier, inc=1, device_id=partner, device_id_type=MESH)
    pl.semaphore_signal(barrier, inc=1, device_id=mirror, device_id_type=MESH)

    for half in (0, 1):
        rows = slice(half * 128, half * 128 + 128)
        g_ref[at["z"], at["y"], at["x"], half, :, 0:128] = small_ref[rows, :]
        g_ref[at["z"], at["y"], at["x"], half, :, 128:384] = large_ref[rows, :]
        c_ref[at["z"], at["y"], at["x"], half * 16 : half * 16 + 16, :] = gates_ref[:, rows]

    def rows_of(piece, kind):
        _, _, first, count, half = pieces[piece]
        if kind == 2:
            return (first, half)
        if kind == 3:
            return (first + half, count - half)
        return (first, count)

    def view(piece, phase, offset, kind, side):
        order = orders[pieces[piece][0]]
        index = []
        for dim in ("z", "y", "x"):
            where = order.index(dim)
            if where < phase:
                index.append(slice(None))
            else:
                index.append((at[dim] + offset) % 4 if where == phase else at[dim])
        rows = pl.ds(*rows_of(piece, kind))
        if pieces[piece][1]:
            return c_ref.at[(*index, rows, slice(None))]
        return g_ref.at[(*index, side, rows, slice(None))]

    def sent(piece, phase, kind):
        target = view(piece, phase, (0, 0, 3, 1)[kind], kind, tp)
        return pltpu.make_async_remote_copy(
            src_ref=target, dst_ref=target, send_sem=send.at[piece, phase, kind], recv_sem=recv.at[piece, phase, kind],
            device_id=moved(orders[pieces[piece][0]][phase], 1 if kind in (0, 2) else 3), device_id_type=MESH)

    def arrived(piece, phase, kind):
        ref = view(piece, phase, shift[kind], kind, tp)
        return pltpu.make_async_remote_copy(
            src_ref=ref, dst_ref=ref, send_sem=send.at[piece, phase, kind], recv_sem=recv.at[piece, phase, kind],
            device_id=partner, device_id_type=MESH)

    def shared(piece, phase, kind, side):
        ref = view(piece, phase, shift[kind], kind, side)
        return pltpu.make_async_remote_copy(
            src_ref=ref, dst_ref=ref, send_sem=dsend.at[piece, phase, kind], recv_sem=drecv.at[piece, phase, kind],
            device_id=partner, device_id_type=MESH)

    far = [
        pltpu.make_async_remote_copy(
            src_ref=source, dst_ref=target, send_sem=far_send.at[k], recv_sem=far_recv.at[k],
            device_id=mirror, device_id_type=MESH)
        for k, (source, target) in enumerate(((gates_ref, far_gates), (qs_ref, far_qs), (ql_ref, far_ql)))
    ]
    count = range(len(pieces))
    pl.semaphore_wait(barrier, 8)
    for piece in count:
        for kind in (0, 1):
            sent(piece, 0, kind).start()

    @pl.when(sp >= 32)
    def _():
        for copy in far:
            copy.start()

    for phase in range(3):
        for piece in count:
            for kind in (0, 1):
                arrived(piece, phase, kind).wait_recv()
                sent(piece, phase, 2 + kind).start()
                if pieces[piece][1] == 0:
                    shared(piece, phase, kind, tp).start()
        for piece in count:
            for kind in (2, 3):
                arrived(piece, phase, kind).wait_recv()
            if phase < 2:
                for kind in (0, 1):
                    sent(piece, phase + 1, kind).start()
            if pieces[piece][1] == 0:
                for kind in (2, 3):
                    shared(piece, phase, kind, tp).start()

    @pl.when(sp >= 32)
    def _():
        for copy in far:
            copy.wait_send()

    @pl.when(sp < 32)
    def _():
        for copy in far:
            copy.wait_recv()

    for phase in range(3):
        for piece in count:
            for kind in range(4):
                sent(piece, phase, kind).wait_send()
                if pieces[piece][1] == 0:
                    shared(piece, phase, kind, tp).wait_send()
                    shared(piece, phase, kind, 1 - tp).wait_recv()


def gather(small, large, gates, qs, ql):
    DMA = pltpu.SemaphoreType.DMA
    shape = (len(pieces), 3, 4)
    V = pl.BlockSpec(memory_space=pltpu.VMEM)
    return pl.pallas_call(
        gather_kernel,
        out_shape=(
            jax.ShapeDtypeStruct((4, 4, 4, 2, 128, 384), bf16),
            jax.ShapeDtypeStruct((4, 4, 4, 32, 128), f32),
            jax.ShapeDtypeStruct((256, 512), bf16),
            jax.ShapeDtypeStruct((256, 512), bf16),
            jax.ShapeDtypeStruct((16, 256), f32),
        ),
        in_specs=[V] * 5,
        out_specs=(V,) * 5,
        scratch_shapes=[DMA(shape), DMA(shape), DMA(shape), DMA(shape), DMA((3,)), DMA((3,))],
        compiler_params=pltpu.CompilerParams(collective_id=0, has_side_effects=True, vmem_limit_bytes=24 * 1024 * 1024),
        name="gather_keys",
    )(small, large, gates, qs, ql)


def attention_kernel(qs_ref, ql_ref, cq_ref, whole_ref, c_ref, o_ref, ml_ref,
                     near, near_sems, tile, vts, vtl, qs, ql, acc_s, acc_l, top, *, diagonal):
    sp = lax.axis_index("sp")
    if diagonal:
        hi, q0 = sp // 4 + 1, sp * 256
        lo = jnp.maximum(hi - own_units, 0)
    else:
        lo, q0 = 0, (63 - sp) * 256
        hi = jnp.where(sp < 32, jnp.maximum((63 - sp) // 4 + 1 - own_units, 0), 0)

    def fetch(i):
        return pltpu.make_async_copy(
            whole_ref.at[pl.ds(pl.multiple_of((hi - 1 - i) * unit, unit), unit), :], near.at[i], near_sems.at[i])

    if diagonal:
        lax.fori_loop(0, hi - lo, lambda i, _: (fetch(i).start(), 0)[1], 0)
    nq = 256
    cs, cl = log2e / 8.0, log2e / math.sqrt(128.0)
    n = hi - lo

    acc_s[...] = jnp.zeros(acc_s.shape, f32)
    acc_l[...] = jnp.zeros(acc_l.shape, f32)
    top[...] = jnp.zeros(top.shape, f32)
    vts[64:80, :] = jnp.ones((16, unit), bf16)
    vtl[128:144, :] = jnp.ones((16, unit), bf16)
    for k in range(4):
        w = slice(k * nq, (k + 1) * nq)
        two = qs_ref[:, k * 128 : (k + 1) * 128].T
        qs[128:192, 2 * k * nq : (2 * k + 1) * nq] = two[0:64, :]
        qs[128:192, (2 * k + 1) * nq : (2 * k + 2) * nq] = two[64:128, :]
        ql[0:128, w] = ql_ref[:, k * 128 : (k + 1) * 128].T
    qs[192:256, :] = jnp.zeros((64, 2048), bf16)
    row = lax.broadcasted_iota(jnp.int32, (128, nq), 0)
    for h in range(12):
        here = cq_ref[h : h + 1, :]
        high = here.astype(bf16).astype(f32)
        rest = here - high
        middle = rest.astype(bf16).astype(f32)
        low = rest - middle
        chosen = jnp.where((row == h) | (row == 16 + h) | (row == 32 + h), -8.0, 0.0)
        chosen = jnp.where(row == 48, 8.0 * high, chosen)
        chosen = jnp.where(row == 49, 8.0 * middle, chosen)
        chosen = jnp.where(row == 50, 8.0 * low, chosen).astype(bf16)
        if h < 8:
            qs[0:128, h * nq : (h + 1) * nq] = chosen
        else:
            ql[128:256, (h - 8) * nq : (h - 7) * nq] = chosen
    size_s = jnp.max(jnp.sum(jnp.abs(qs[128:192, :].astype(f32)), axis=0, keepdims=True))
    size_l = jnp.max(jnp.sum(jnp.abs(ql[0:128, :].astype(f32)), axis=0, keepdims=True))
    bounded = (size_s <= 150.0) & (size_l <= 210.0)

    def ready(i):
        u = hi - 1 - i
        if diagonal:
            fetch(i).wait()
            here = near.at[i]
        else:
            here = whole_ref.at[pl.ds(pl.multiple_of(u * unit, unit), unit), :]
        for j in range(8):
            gate = c_ref[u * 4 + j // 2, (j % 2) * 16 : (j % 2) * 16 + 16, :]
            high = gate.astype(bf16).astype(f32)
            rest = gate - high
            middle = rest.astype(bf16).astype(f32)
            wide = jnp.concatenate([high, middle, rest - middle, jnp.ones((8, 128), f32), jnp.zeros((72, 128), f32)], axis=0)
            tile[j * 128 : (j + 1) * 128, :] = wide.T.astype(bf16)
        vts[0:64, :] = here[:, 0:128].T[64:128, :]
        vtl[0:128, :] = here[:, 256:384].T
        return u, here

    def keys_small(here):
        return jnp.concatenate([tile[...], here[:, 0:128]], axis=1)

    def keys_large(here):
        return jnp.concatenate([here[:, 128:256], tile[...]], axis=1)

    def allowed(u, width):
        key = u * unit + lax.broadcasted_iota(jnp.int32, (unit, width), 0)
        query = q0 + (lax.broadcasted_iota(jnp.int32, (unit, width), 1) & (nq - 1))
        return key <= query

    def quick(i, masked):
        u, here = ready(i)
        for keys, q, w, vt, acc, scale in (
            (keys_small, qs, 0, vts, acc_s, cs),
            (keys_small, qs, 1024, vts, acc_s, cs),
            (keys_large, ql, 0, vtl, acc_l, cl),
        ):
            s = jnp.dot(keys(here), q[:, w : w + 1024], preferred_element_type=f32) * scale
            if masked:
                s = jnp.where(allowed(u, 1024), s, far_score)
            p = jnp.exp2(s).astype(bf16)
            acc[:, w : w + 1024] += jnp.dot(vt[...], p, preferred_element_type=f32)

    def careful(i, _):
        u, here = ready(i)

        def group(keys, q, vt, acc, scale, count, base):
            def head(h, _):
                w = pl.ds(pl.multiple_of(h * nq, nq), nq)
                s = jnp.dot(keys(here), q[:, w], preferred_element_type=f32) * scale
                s = jnp.where(allowed(u, nq), s, far_score)
                before = top[base + h]
                after = jnp.maximum(before, jnp.max(s, axis=0, keepdims=True))
                top[base + h] = after
                p = jnp.exp2(s - after).astype(bf16)
                acc[:, w] = acc[:, w] * jnp.exp2(before - after) + jnp.dot(vt[...], p, preferred_element_type=f32)
                return 0

            lax.fori_loop(0, count, head, 0)

        group(keys_small, qs, vts, acc_s, cs, 8, 0)
        group(keys_large, ql, vtl, acc_l, cl, 4, 8)
        return 0

    @pl.when(bounded)
    def _():
        if diagonal:
            quick(0, True)
        lax.fori_loop(1 if diagonal else 0, n, lambda i, _: (quick(i, False), 0)[1], 0)

    @pl.when(jnp.logical_not(bounded))
    def _():
        top[...] = jnp.full(top.shape, far_score, f32)
        lax.fori_loop(0, n, careful, 0)

    ml_ref[...] = jnp.zeros(ml_ref.shape, f32)
    for h in range(12):
        size, acc, base, k = (64, acc_s, 0, h) if h < 8 else (128, acc_l, 512, h - 8)
        w = slice(k * nq, (k + 1) * nq)
        total = acc[size : size + 1, w]
        scale = jnp.where(total > 0, 1.0 / jnp.where(total > 0, total, 1.0), 0.0)
        o_ref[base + k * size : base + (k + 1) * size, :] = (acc[0:size, w] * scale).astype(o_ref.dtype)
        ml_ref[h : h + 1, :] = top[h]
        ml_ref[16 + h : 17 + h, :] = total


def attention(qs, ql, cq, g, c, diagonal):
    V = pl.BlockSpec(memory_space=pltpu.VMEM)
    kind = f32 if diagonal else bf16
    VM = pltpu.VMEM
    return pl.pallas_call(
        functools.partial(attention_kernel, diagonal=diagonal),
        out_shape=(
            jax.ShapeDtypeStruct((1024, 256), kind),
            jax.ShapeDtypeStruct((32, 256), f32),
        ),
        in_specs=[V] * 3 + [pl.BlockSpec(memory_space=pltpu.HBM) if diagonal else V, V],
        out_specs=(V, V),
        scratch_shapes=[
            VM((own_units if diagonal else 1, unit, 384), bf16), pltpu.SemaphoreType.DMA((own_units,)), VM((unit, 128), bf16),
            VM((80, unit), bf16), VM((144, unit), bf16), VM((256, 2048), bf16), VM((256, 1024), bf16),
            VM((80, 2048), f32), VM((144, 1024), f32), VM((12, 1, 256), f32),
        ],
        compiler_params=pltpu.CompilerParams(vmem_limit_bytes=36 * 1024 * 1024),
        cost_estimate=pl.CostEstimate(flops=12_000_000_000 if diagonal else 8_000_000_000, bytes_accessed=12_000_000, transcendentals=26_000_000),
        name="attention_own" if diagonal else "attention_far",
    )(qs, ql, cq, g, c)


def merged(own, far, m_own, m_far, l_own, l_far, heads):
    m_far = jnp.where(l_far > 0, m_far, far_score)
    most = jnp.maximum(m_own, m_far)
    a, b = l_own * jnp.exp2(m_own - most), l_far * jnp.exp2(m_far - most)
    whole = a + b
    size = own.shape[0] // heads
    own = own.reshape(heads, size, 256) * (a / whole)[:, None, :]
    far = far.astype(f32).reshape(heads, size, 256) * (b / whole)[:, None, :]
    return (own + far).astype(bf16).reshape(heads * size, 256)


def reach(offset):
    return sum((0, 1, 2, 1)[(offset // step) % 4] for step in (1, 4, 16))


offsets = tuple(sorted(range(1, 64), key=lambda offset: -reach(offset)))


def expert_kernel(part_ref, residual_ref, mix_ref, route_ref, blend_ref, table_ref, weight_ref, gate_hbm, up_hbm, down_hbm, out_ref,
                  gate_w, up_w, down_w, other, rows, leaving, taken, hidden, made, back, kept, given, swapped,
                  load, pair_send, pair_recv, go_send, go_recv, back_send, back_recv):
    sp, tp = lax.axis_index("sp"), lax.axis_index("tp")
    z, y, x = sp // 16, (sp // 4) % 4, sp % 4

    def chip(offset, sign):
        oz, oy, ox = offset // 16, (offset // 4) % 4, offset % 4
        return ((z + sign * oz + 4) % 4) * 16 + ((y + sign * oy + 4) % 4) * 4 + (x + sign * ox + 4) % 4

    partner = (sp, 1 - tp)
    loads = [
        pltpu.make_async_copy(source.at[0], target, load.at[k])
        for k, (source, target) in enumerate(((gate_hbm, gate_w), (up_hbm, up_w), (down_hbm, down_w)))
    ]
    barrier = pltpu.get_barrier_semaphore()
    for offset in offsets:
        pl.semaphore_signal(barrier, inc=1, device_id=(chip(offset, 1), tp), device_id_type=MESH)
    pl.semaphore_signal(barrier, inc=1, device_id=partner, device_id_type=MESH)
    for copy in loads:
        copy.start()
    pl.semaphore_wait(barrier, 64)

    def across(source, target, k):
        return pltpu.make_async_remote_copy(
            src_ref=source, dst_ref=target, send_sem=pair_send.at[k], recv_sem=pair_recv.at[k],
            device_id=partner, device_id_type=MESH)

    first = across(part_ref.at[pl.ds((1 - tp) * 128, 128), :], other, 0)
    first.start()
    first.wait()

    def scaled(values, gain):
        return values * lax.rsqrt(jnp.mean(values * values, axis=-1, keepdims=True) + norm_eps) * gain

    mixer = part_ref[pl.ds(pl.multiple_of(tp * 128, 128), 128), :].astype(f32) + other[...].astype(f32)
    mixed = (residual_ref[...].astype(f32) + scaled(mixer, mix_ref[...])).astype(bf16)
    kept[...] = mixed
    given[...] = scaled(mixed.astype(f32), route_ref[...]).astype(bf16)
    mine = pl.ds(pl.multiple_of(tp * 128, 128), 128)
    rows[mine, :] = given[...]
    second = across(given, rows.at[mine, :], 1)
    second.start()
    second.wait_send()
    theirs = rows.at[pl.ds(pl.multiple_of((1 - tp) * 128, 128), 128), :]
    across(theirs, theirs, 1).wait_recv()
    for w in range(0, 2048, 512):
        leaving[:, :, w : w + 512] = jnp.dot(table_ref[...], rows[:, w : w + 512], preferred_element_type=f32).astype(bf16).reshape(64, 8, 512)

    def go(n):
        return pltpu.make_async_remote_copy(
            src_ref=leaving.at[chip(offsets[n], 1)], dst_ref=taken.at[n], send_sem=go_send.at[n], recv_sem=go_recv.at[n],
            device_id=(chip(offsets[n], 1), tp), device_id_type=MESH)

    def come(n):
        return pltpu.make_async_remote_copy(
            src_ref=made.at[n], dst_ref=back.at[sp], send_sem=back_send.at[n], recv_sem=back_recv.at[n],
            device_id=(chip(offsets[n], -1), tp), device_id_type=MESH)

    def came(n):
        ref = back.at[chip(offsets[n], 1)]
        return pltpu.make_async_remote_copy(
            src_ref=ref, dst_ref=ref, send_sem=back_send.at[n], recv_sem=back_recv.at[n], device_id=partner, device_id_type=MESH)

    for n in range(63):
        go(n).start()
    taken[63] = leaving[sp]
    for copy in loads:
        copy.wait()
    for group in (0, 1):
        members = range(32 * group, min(32 * group + 32, 63))
        for n in members:
            go(n).wait_recv()
        arrivals = taken[32 * group : 32 * group + 32].reshape(256, 2048)

        def widen(k, _):
            w = pl.ds(pl.multiple_of(k * 256, 256), 256)
            gated = jnp.dot(arrivals, gate_w[:, w], preferred_element_type=f32)
            upped = jnp.dot(arrivals, up_w[:, w], preferred_element_type=f32)
            hidden[:, w] = (gated / (1.0 + jnp.exp(-gated)) * upped).astype(bf16)
            return 0

        lax.fori_loop(0, 4, widen, 0)

        def narrow(k, _):
            w = pl.ds(pl.multiple_of(k * 512, 512), 512)
            made[32 * group : 32 * group + 32, :, w] = jnp.dot(hidden[...], down_w[:, w], preferred_element_type=f32).astype(bf16).reshape(32, 8, 512)
            return 0

        lax.fori_loop(0, 4, narrow, 0)
        for n in members:
            come(n).start()
    back[sp] = made[63]
    for n in range(63):
        go(n).wait_send()
    for n in range(63):
        came(n).wait_recv()
    for n in range(63):
        come(n).wait_send()
    ours = pl.ds(pl.multiple_of(tp * 128, 128), 128)
    away = pl.ds(pl.multiple_of((1 - tp) * 128, 128), 128)

    for w in range(0, 2048, 512):
        returned = back[:, :, w : w + 512].reshape(512, 512)
        given[:, w : w + 512] = (
            jnp.dot(weight_ref[away, 0:512], returned, preferred_element_type=f32)
            + jnp.dot(weight_ref[away, 512:1024], returned, preferred_element_type=f32)
        ).astype(bf16)
    third = across(given, swapped, 2)
    third.start()
    parts = []
    for w in range(0, 2048, 512):
        returned = back[:, :, w : w + 512].reshape(512, 512)
        parts.append(
            jnp.dot(weight_ref[ours, 0:512], returned, preferred_element_type=f32)
            + jnp.dot(weight_ref[ours, 512:1024], returned, preferred_element_type=f32)
        )
    third.wait()
    blended = jnp.concatenate(parts, axis=1) + swapped[...].astype(f32)
    out_ref[...] = (kept[...].astype(f32) + scaled(blended, blend_ref[...])).astype(bf16)


def experts(part, residual, gain_mix, gain_route, gain_blend, table, weight, w_gate, w_up, w_down):
    V = pl.BlockSpec(memory_space=pltpu.VMEM)
    A = pl.BlockSpec(memory_space=pl.ANY)
    VM, DMA = pltpu.VMEM, pltpu.SemaphoreType.DMA
    return pl.pallas_call(
        expert_kernel,
        out_shape=jax.ShapeDtypeStruct((128, 2048), bf16),
        in_specs=[V] * 7 + [A] * 3,
        out_specs=V,
        scratch_shapes=[
            VM((2048, 1024), bf16), VM((2048, 1024), bf16), VM((1024, 2048), bf16),
            VM((128, 2048), bf16), VM((256, 2048), bf16), VM((64, 8, 2048), bf16), VM((64, 8, 2048), bf16),
            VM((256, 1024), bf16), VM((64, 8, 2048), bf16), VM((64, 8, 2048), bf16),
            VM((128, 2048), bf16), VM((128, 2048), bf16), VM((128, 2048), bf16),
            DMA((3,)), DMA((3,)), DMA((3,)), DMA((64,)), DMA((64,)), DMA((64,)), DMA((64,)),
        ],
        compiler_params=pltpu.CompilerParams(collective_id=1, has_side_effects=True, vmem_limit_bytes=50 * 1024 * 1024),
        name="experts",
    )(part, residual, gain_mix, gain_route, gain_blend, table, weight, w_gate, w_up, w_down)


def routing(route, route_bias, tp):
    def both(a):
        theirs = lax.ppermute(a, "tp", [(0, 1), (1, 0)])
        return jnp.where(tp == 0, jnp.stack([a, theirs]), jnp.stack([theirs, a]))

    ids = both(route).reshape(2, 256)
    bias = both(route_bias)
    marked = (ids[:, :, None] == jnp.arange(128, dtype=jnp.int32)).astype(bf16)
    before = (jnp.arange(256)[:, None] > jnp.arange(256)[None, :]).astype(bf16)
    counts = jnp.einsum("ij,cje->cie", before, marked, preferred_element_type=f32)
    rank = jnp.sum(counts * marked.astype(f32), axis=2).astype(jnp.int32)
    slot = jnp.where(ids % 2 == tp, ids // 2 * 8 + jnp.arange(2, dtype=jnp.int32)[:, None] * 4 + rank, -1).reshape(2, 2, 128)
    places = jnp.arange(512, dtype=jnp.int32)
    to_slot = slot.transpose(1, 0, 2).reshape(2, 256)
    table = ((places[:, None] == to_slot[0][None, :]) | (places[:, None] == to_slot[1][None, :])).astype(bf16)
    share = jnp.stack([jax.nn.sigmoid(bias), jax.nn.sigmoid(-bias)]).reshape(2, 256)
    weight = sum(jnp.where(to_slot[k][:, None] == places[None, :], share[k][:, None], 0.0) for k in range(2))
    high = lax.reduce_precision(weight, 8, 7)
    return table, jnp.concatenate([high, weight - high], axis=1).astype(bf16)


def on_device(
    queries_small,
    queries_large,
    kv_small,
    kv_large,
    cum_small,
    cum_large,
    residual,
    out_small,
    out_large,
    gain_mix,
    gain_route,
    gain_blend,
    w_gate,
    w_up,
    w_down,
    route,
    route_bias,
):
    tp = lax.axis_index("tp")
    chips = lax.axis_size("sp")
    gates = jnp.concatenate([cum_small, cum_large * jnp.float32(math.sqrt(2.0)), jnp.zeros((4, 256), f32)], axis=0)
    to_late = [(i, chips - 1 - i) for i in range(chips // 2)]
    g, c, *far_q = gather(kv_small, kv_large, gates, queries_small, queries_large)
    g, c = g.reshape(chips * 256, 384), c.reshape(chips, 32, 128)
    far_o, far_ml = attention(*far_q, g, c, False)
    far_o = lax.ppermute(far_o, "sp", to_late)
    far_ml = lax.ppermute(far_ml, "sp", to_late)
    own_o, own_ml = attention(queries_small, queries_large, gates, g, c, True)
    attn_small = merged(own_o[0:512], far_o[0:512], own_ml[0:8], far_ml[0:8], own_ml[16:24], far_ml[16:24], 8)
    attn_large = merged(own_o[512:], far_o[512:], own_ml[8:12], far_ml[8:12], own_ml[24:28], far_ml[24:28], 4)
    weight_small = lax.dynamic_slice_in_dim(
        out_small, tp * 512, 512, 0
    )
    weight_large = lax.dynamic_slice_in_dim(
        out_large, tp * 512, 512, 0
    )
    part = (
        lax.dot_general(attn_small, weight_small, (((0,), (0,)), ((), ())), preferred_element_type=f32)
        + lax.dot_general(attn_large, weight_large, (((0,), (0,)), ((), ())), preferred_element_type=f32)
    ).astype(bf16)
    table, weight = routing(route, route_bias, tp)
    return experts(
        part, residual, gain_mix[None], gain_route[None], gain_blend[None], table, weight, w_gate, w_up, w_down
    )


def solution(mesh):
    in_specs = (
        P("sp", "tp"),
        P("sp", "tp"),
        P("sp", None),
        P("sp", None),
        P("tp", "sp"),
        P("tp", "sp"),
        P(("sp", "tp"), None),
        P(),
        P(),
        P(),
        P(),
        P(),
        P(("sp", "tp"), None, None),
        P(("sp", "tp"), None, None),
        P(("sp", "tp"), None, None),
        P(None, ("sp", "tp")),
        P(("sp", "tp")),
    )
    out_specs = P(("sp", "tp"), None)
    return jax.shard_map(
        on_device, mesh=mesh, in_specs=in_specs, out_specs=out_specs, check_vma=False
    )
```

```python
import functools
import math

import jax
import jax.numpy as jnp
from jax import lax
from jax.experimental import pallas as pl
from jax.experimental.pallas import tpu as pltpu
from jax.sharding import PartitionSpec as P


MESH = pl.DeviceIdType.MESH
norm_eps = 1e-06
far_score = -1e30
log2e = 1.4426950408889634
f32, bf16 = jnp.float32, jnp.bfloat16
unit = 1024
own_units = 10

orders = (("x", "y", "z"), ("y", "z", "x"), ("z", "x", "y"))
pieces = (
    (0, 0, 0, 32, 16),
    (1, 0, 48, 32, 16),
    (2, 0, 96, 32, 16),
    (0, 0, 32, 16, 8),
    (1, 0, 80, 16, 8),
    (2, 1, 0, 32, 16),
)
shift = (3, 1, 2, 2)


def routing(ids_ref, bias_ref, table_ref, weight_ref, tp):
    expert = lax.broadcasted_iota(jnp.int32, (128, 128), 0)
    earlier = (expert < lax.broadcasted_iota(jnp.int32, (128, 128), 1)).astype(bf16)
    place = lax.broadcasted_iota(jnp.int32, (512, 128), 0)
    for core in range(2):
        table = jnp.zeros((512, 128), f32)
        weight = jnp.zeros((512, 128), f32)
        taken = jnp.zeros((128, 1), f32)
        for k in range(2):
            ids = ids_ref[core, k : k + 1, :]
            marked = (expert == ids).astype(f32)
            counts = jnp.dot(marked.astype(bf16), earlier, preferred_element_type=f32) + taken
            taken = taken + jnp.sum(marked, axis=1, keepdims=True)
            rank = jnp.sum(marked * counts, axis=0, keepdims=True).astype(jnp.int32)
            slot = jnp.where((ids & 1) == tp, (ids >> 1) * 8 + core * 4 + rank, -1)
            bias = bias_ref[core]
            share = 1.0 / (1.0 + jnp.exp(-bias if k == 0 else bias))
            here = place == slot
            table = jnp.where(here, 1.0, table)
            weight = jnp.where(here, share, weight)
        columns = slice(core * 128, core * 128 + 128)
        table_ref[:, columns] = table.astype(bf16)
        turned = weight.T
        high = turned.astype(bf16)
        weight_ref[columns, 0:512] = high
        weight_ref[columns, 512:1024] = (turned - high.astype(f32)).astype(bf16)


def gather_kernel(small_ref, large_ref, cum_s_ref, cum_l_ref, qs_ref, ql_ref, route_ref, bias_ref,
                  g_ref, c_ref, far_qs, far_ql, far_gates, table_ref, weight_ref, gates_ref,
                  ids, biases, own, own_sems, send, recv, dsend, drecv, far_send, far_recv, pair_send, pair_recv):
    sp, tp = lax.axis_index("sp"), lax.axis_index("tp")
    at = {"z": sp // 16, "y": (sp // 4) % 4, "x": sp % 4}
    partner = (sp, 1 - tp)
    mirror = (63 - sp, tp)
    far_qs[...] = jnp.zeros(far_qs.shape, bf16)
    far_ql[...] = jnp.zeros(far_ql.shape, bf16)
    far_gates[...] = jnp.zeros(far_gates.shape, f32)

    def moved(dim, by):
        here = dict(at)
        here[dim] = (at[dim] + by) % 4
        return (here["z"] * 16 + here["y"] * 4 + here["x"], tp)

    barrier = pltpu.get_barrier_semaphore()
    for dim in ("x", "y", "z"):
        for by in (1, 3):
            pl.semaphore_signal(barrier, inc=1, device_id=moved(dim, by), device_id_type=MESH)
    pl.semaphore_signal(barrier, inc=1, device_id=partner, device_id_type=MESH)
    pl.semaphore_signal(barrier, inc=1, device_id=mirror, device_id_type=MESH)

    gates_ref[...] = jnp.concatenate([cum_s_ref[...], cum_l_ref[...] * jnp.float32(math.sqrt(2.0)), jnp.zeros((4, 256), f32)], axis=0)
    staged, placed = [], []
    for half in (0, 1):
        rows = pl.ds(half * 128, 128)
        staged.append(pltpu.make_async_copy(small_ref.at[rows, :], own.at[half, :, pl.ds(0, 128)], own_sems.at[half]))
        staged.append(pltpu.make_async_copy(large_ref.at[rows, :], own.at[half, :, pl.ds(128, 256)], own_sems.at[2 + half]))
        placed.append(pltpu.make_async_copy(own.at[half], g_ref.at[at["z"], at["y"], at["x"], half], own_sems.at[4 + half]))
        c_ref[at["z"], at["y"], at["x"], half * 16 : half * 16 + 16, :] = gates_ref[:, half * 128 : half * 128 + 128]
    for copy in staged:
        copy.start()
    ids[tp] = route_ref[...]
    biases[tp] = bias_ref[...]
    pairs = [
        pltpu.make_async_remote_copy(
            src_ref=source, dst_ref=whole.at[tp], send_sem=pair_send.at[k], recv_sem=pair_recv.at[k],
            device_id=partner, device_id_type=MESH)
        for k, (source, whole) in enumerate(((route_ref, ids), (bias_ref, biases)))
    ]
    paired = [
        pltpu.make_async_remote_copy(
            src_ref=whole.at[1 - tp], dst_ref=whole.at[1 - tp], send_sem=pair_send.at[k], recv_sem=pair_recv.at[k],
            device_id=partner, device_id_type=MESH)
        for k, whole in enumerate((ids, biases))
    ]

    def rows_of(piece, kind):
        _, _, first, count, half = pieces[piece]
        if kind == 2:
            return (first, half)
        if kind == 3:
            return (first + half, count - half)
        return (first, count)

    def view(piece, phase, offset, kind, side):
        order = orders[pieces[piece][0]]
        index = []
        for dim in ("z", "y", "x"):
            where = order.index(dim)
            if where < phase:
                index.append(slice(None))
            else:
                index.append((at[dim] + offset) % 4 if where == phase else at[dim])
        rows = pl.ds(*rows_of(piece, kind))
        if pieces[piece][1]:
            return c_ref.at[(*index, rows, slice(None))]
        return g_ref.at[(*index, side, rows, slice(None))]

    def sent(piece, phase, kind):
        target = view(piece, phase, (0, 0, 3, 1)[kind], kind, tp)
        source = target
        if phase == 0 and kind < 2 and pieces[piece][1] == 0:
            source = own.at[tp, pl.ds(*rows_of(piece, kind)), :]
        return pltpu.make_async_remote_copy(
            src_ref=source, dst_ref=target, send_sem=send.at[piece, phase, kind], recv_sem=recv.at[piece, phase, kind],
            device_id=moved(orders[pieces[piece][0]][phase], 1 if kind in (0, 2) else 3), device_id_type=MESH)

    def arrived(piece, phase, kind):
        ref = view(piece, phase, shift[kind], kind, tp)
        return pltpu.make_async_remote_copy(
            src_ref=ref, dst_ref=ref, send_sem=send.at[piece, phase, kind], recv_sem=recv.at[piece, phase, kind],
            device_id=partner, device_id_type=MESH)

    def shared(piece, phase, kind, side):
        ref = view(piece, phase, shift[kind], kind, side)
        return pltpu.make_async_remote_copy(
            src_ref=ref, dst_ref=ref, send_sem=dsend.at[piece, phase, kind], recv_sem=drecv.at[piece, phase, kind],
            device_id=partner, device_id_type=MESH)

    far = [
        pltpu.make_async_remote_copy(
            src_ref=source, dst_ref=target, send_sem=far_send.at[k], recv_sem=far_recv.at[k],
            device_id=mirror, device_id_type=MESH)
        for k, (source, target) in enumerate(((gates_ref, far_gates), (qs_ref, far_qs), (ql_ref, far_ql)))
    ]
    count = range(len(pieces))
    for copy in staged:
        copy.wait()
    for copy in placed:
        copy.start()
    pl.semaphore_wait(barrier, 8)
    for piece in count:
        for kind in (0, 1):
            sent(piece, 0, kind).start()

    @pl.when(sp >= 32)
    def _():
        for copy in far:
            copy.start()

    for copy in pairs:
        copy.start()
    for copy in placed:
        copy.wait()
    for phase in range(3):
        if phase == 2:
            for copy in paired:
                copy.wait_recv()
            routing(ids, biases, table_ref, weight_ref, tp)
        for piece in count:
            for kind in (0, 1):
                arrived(piece, phase, kind).wait_recv()
                sent(piece, phase, 2 + kind).start()
                if pieces[piece][1] == 0:
                    shared(piece, phase, kind, tp).start()
        for piece in count:
            for kind in (2, 3):
                arrived(piece, phase, kind).wait_recv()
            if phase < 2:
                for kind in (0, 1):
                    sent(piece, phase + 1, kind).start()
            if pieces[piece][1] == 0:
                for kind in (2, 3):
                    shared(piece, phase, kind, tp).start()

    for copy in pairs:
        copy.wait_send()

    @pl.when(sp >= 32)
    def _():
        for copy in far:
            copy.wait_send()

    @pl.when(sp < 32)
    def _():
        for copy in far:
            copy.wait_recv()

    for phase in range(3):
        for piece in count:
            for kind in range(4):
                sent(piece, phase, kind).wait_send()
                if pieces[piece][1] == 0:
                    shared(piece, phase, kind, tp).wait_send()
                    shared(piece, phase, kind, 1 - tp).wait_recv()


def gather(small, large, cum_s, cum_l, qs, ql, route, bias):
    DMA = pltpu.SemaphoreType.DMA
    shape = (len(pieces), 3, 4)
    V = pl.BlockSpec(memory_space=pltpu.VMEM)
    A = pl.BlockSpec(memory_space=pl.ANY)
    return pl.pallas_call(
        gather_kernel,
        out_shape=(
            jax.ShapeDtypeStruct((4, 4, 4, 2, 128, 384), bf16),
            jax.ShapeDtypeStruct((4, 4, 4, 32, 128), f32),
            jax.ShapeDtypeStruct((256, 512), bf16),
            jax.ShapeDtypeStruct((256, 512), bf16),
            jax.ShapeDtypeStruct((16, 256), f32),
            jax.ShapeDtypeStruct((512, 256), bf16),
            jax.ShapeDtypeStruct((256, 1024), bf16),
            jax.ShapeDtypeStruct((16, 256), f32),
        ),
        in_specs=[A, A, V, V, A, A, V, V],
        out_specs=(A,) + (V,) * 7,
        scratch_shapes=[
            pltpu.VMEM((2, 2, 128), jnp.int32), pltpu.VMEM((2, 1, 128), f32), pltpu.VMEM((2, 128, 384), bf16), DMA((6,)),
            DMA(shape), DMA(shape), DMA(shape), DMA(shape), DMA((3,)), DMA((3,)), DMA((2,)), DMA((2,)),
        ],
        compiler_params=pltpu.CompilerParams(collective_id=0, has_side_effects=True, vmem_limit_bytes=60 * 1024 * 1024),
        name="gather_keys",
    )(small, large, cum_s, cum_l, qs, ql, route, bias)


def attention_kernel(qs_hbm, ql_hbm, cq_ref, whole_ref, c_ref, *refs, diagonal):
    if diagonal:
        o_ref, ml_ref, *scratch = refs
    else:
        (o_ref, *scratch), ml_ref = refs, None
    attend(qs_hbm, ql_hbm, cq_ref, whole_ref, c_ref, o_ref, ml_ref, *scratch, diagonal=diagonal)


def split3(values):
    high = values.astype(bf16).astype(f32)
    rest = values - high
    middle = rest.astype(bf16).astype(f32)
    return high, middle, rest - middle


def attend(qs_hbm, ql_hbm, cq_ref, whole_ref, c_ref, o_ref, ml_ref,
                     qs_ref, ql_ref, query_sems, near, near_sems, tile, vts, vtl, qs, ql, acc_s, acc_l, top, *, diagonal):
    sp = lax.axis_index("sp")
    if diagonal:
        hi, q0 = sp // 4 + 1, sp * 256
        lo = jnp.maximum(hi - own_units, 0)
    else:
        lo, q0 = 0, (63 - sp) * 256
        hi = jnp.where(sp < 32, jnp.maximum((63 - sp) // 4 + 1 - own_units, 0), 0)

    def fetch(i):
        return pltpu.make_async_copy(
            whole_ref.at[pl.ds(pl.multiple_of((hi - 1 - i) * unit, unit), unit), :], near.at[i], near_sems.at[i])

    n = hi - lo

    @pl.when(n > 0)
    def _():
        queries = [
            pltpu.make_async_copy(qs_hbm, qs_ref, query_sems.at[0]),
            pltpu.make_async_copy(ql_hbm, ql_ref, query_sems.at[1]),
        ]
        for copy in queries:
            copy.start()
        lax.fori_loop(0, hi - lo, lambda i, _: (fetch(i).start(), 0)[1], 0)
        nq = 256
        cs, cl = log2e / 8.0, log2e / math.sqrt(128.0)

        acc_s[...] = jnp.zeros(acc_s.shape, f32)
        acc_l[...] = jnp.zeros(acc_l.shape, f32)
        top[...] = jnp.zeros(top.shape, f32)
        vts[64:80, :] = jnp.ones((16, unit), bf16)
        vtl[128:144, :] = jnp.ones((16, unit), bf16)
        for copy in queries:
            copy.wait()
        for k in range(4):
            w = slice(k * nq, (k + 1) * nq)
            two = qs_ref[:, k * 128 : (k + 1) * 128].T
            qs[128:192, 2 * k * nq : (2 * k + 1) * nq] = two[0:64, :]
            qs[128:192, (2 * k + 1) * nq : (2 * k + 2) * nq] = two[64:128, :]
            ql[0:128, w] = ql_ref[:, k * 128 : (k + 1) * 128].T
        qs[192:256, :] = jnp.zeros((64, 2048), bf16)
        row = lax.broadcasted_iota(jnp.int32, (128, nq), 0)
        for h in range(12):
            here = cq_ref[h : h + 1, :]
            high = here.astype(bf16).astype(f32)
            rest = here - high
            middle = rest.astype(bf16).astype(f32)
            low = rest - middle
            chosen = jnp.where((row == h) | (row == 16 + h) | (row == 32 + h), -8.0, 0.0)
            chosen = jnp.where(row == 48, 8.0 * high, chosen)
            chosen = jnp.where(row == 49, 8.0 * middle, chosen)
            chosen = jnp.where(row == 50, 8.0 * low, chosen).astype(bf16)
            if h < 8:
                qs[0:128, h * nq : (h + 1) * nq] = chosen
            else:
                ql[128:256, (h - 8) * nq : (h - 7) * nq] = chosen
        size_s = jnp.max(jnp.sum(jnp.abs(qs[128:192, :].astype(f32)), axis=0, keepdims=True))
        size_l = jnp.max(jnp.sum(jnp.abs(ql[0:128, :].astype(f32)), axis=0, keepdims=True))
        bounded = (size_s <= 150.0) & (size_l <= 210.0)

        def ready(i):
            u = hi - 1 - i
            fetch(i).wait()
            here = near.at[i]
            for j in range(8):
                gate = c_ref[u * 4 + j // 2, (j % 2) * 16 : (j % 2) * 16 + 16, :]
                high = gate.astype(bf16).astype(f32)
                rest = gate - high
                middle = rest.astype(bf16).astype(f32)
                wide = jnp.concatenate([high, middle, rest - middle, jnp.ones((8, 128), f32), jnp.zeros((72, 128), f32)], axis=0)
                tile[j * 128 : (j + 1) * 128, :] = wide.T.astype(bf16)
            vts[0:64, :] = here[:, 0:128].T[64:128, :]
            vtl[0:128, :] = here[:, 256:384].T
            return u, here

        def keys_small(here):
            return jnp.concatenate([tile[...], here[:, 0:128]], axis=1)

        def keys_large(here):
            return jnp.concatenate([here[:, 128:256], tile[...]], axis=1)

        def allowed(u, width):
            key = u * unit + lax.broadcasted_iota(jnp.int32, (unit, width), 0)
            query = q0 + (lax.broadcasted_iota(jnp.int32, (unit, width), 1) & (nq - 1))
            return key <= query

        def quick(i, masked):
            u, here = ready(i)
            for keys, q, w, vt, acc, scale in (
                (keys_small, qs, 0, vts, acc_s, cs),
                (keys_small, qs, 1024, vts, acc_s, cs),
                (keys_large, ql, 0, vtl, acc_l, cl),
            ):
                s = jnp.dot(keys(here), q[:, w : w + 1024], preferred_element_type=f32) * scale
                if masked:
                    s = jnp.where(allowed(u, 1024), s, far_score)
                p = jnp.exp2(s).astype(bf16)
                acc[:, w : w + 1024] += jnp.dot(vt[...], p, preferred_element_type=f32)

        def careful(i, _):
            u, here = ready(i)

            def group(keys, q, vt, acc, scale, count, base):
                def head(h, _):
                    w = pl.ds(pl.multiple_of(h * nq, nq), nq)
                    s = jnp.dot(keys(here), q[:, w], preferred_element_type=f32) * scale
                    s = jnp.where(allowed(u, nq), s, far_score)
                    before = top[base + h]
                    after = jnp.maximum(before, jnp.max(s, axis=0, keepdims=True))
                    top[base + h] = after
                    p = jnp.exp2(s - after).astype(bf16)
                    acc[:, w] = acc[:, w] * jnp.exp2(before - after) + jnp.dot(vt[...], p, preferred_element_type=f32)
                    return 0

                lax.fori_loop(0, count, head, 0)

            group(keys_small, qs, vts, acc_s, cs, 8, 0)
            group(keys_large, ql, vtl, acc_l, cl, 4, 8)
            return 0

        @pl.when(bounded)
        def _():
            if diagonal:
                quick(0, True)
            lax.fori_loop(1 if diagonal else 0, n, lambda i, _: (quick(i, False), 0)[1], 0)

        @pl.when(jnp.logical_not(bounded))
        def _():
            top[...] = jnp.full(top.shape, far_score, f32)
            lax.fori_loop(0, n, careful, 0)

        tops, totals = [], []
        for h in range(12):
            size, acc, base, k = (64, acc_s, 0, h) if h < 8 else (128, acc_l, 512, h - 8)
            w = slice(k * nq, (k + 1) * nq)
            total = acc[size : size + 1, w]
            scale = jnp.where(total > 0, 1.0 / jnp.where(total > 0, total, 1.0), 0.0)
            o_ref[base + k * size : base + (k + 1) * size, :] = (acc[0:size, w] * scale).astype(o_ref.dtype)
            tops.append(top[h])
            totals.append(total)
        blank = jnp.zeros((4, nq), f32)
        ml = jnp.concatenate(tops + [blank] + totals + [blank], axis=0)
        if diagonal:
            ml_ref[...] = ml
        else:
            for k, piece in enumerate(split3(ml)):
                o_ref[1024 + 32 * k : 1056 + 32 * k, :] = piece.astype(bf16)

    @pl.when(n == 0)
    def _():
        o_ref[...] = jnp.zeros(o_ref.shape, o_ref.dtype)


def attention(qs, ql, cq, g, c, diagonal):
    V = pl.BlockSpec(memory_space=pltpu.VMEM)
    A = pl.BlockSpec(memory_space=pl.ANY)
    kind = f32 if diagonal else bf16
    VM = pltpu.VMEM
    return pl.pallas_call(
        functools.partial(attention_kernel, diagonal=diagonal),
        out_shape=(
            (jax.ShapeDtypeStruct((1024, 256), kind), jax.ShapeDtypeStruct((32, 256), f32))
            if diagonal
            else jax.ShapeDtypeStruct((1120, 256), kind)
        ),
        in_specs=[A, A, V, A, V],
        out_specs=(V, V) if diagonal else V,
        scratch_shapes=[
            VM((256, 512), bf16), VM((256, 512), bf16), pltpu.SemaphoreType.DMA((2,)),
            VM((own_units, unit, 384), bf16), pltpu.SemaphoreType.DMA((own_units,)), VM((unit, 128), bf16),
            VM((80, unit), bf16), VM((144, unit), bf16), VM((256, 2048), bf16), VM((256, 1024), bf16),
            VM((80, 2048), f32), VM((144, 1024), f32), VM((12, 1, 256), f32),
        ],
        compiler_params=pltpu.CompilerParams(vmem_limit_bytes=(52 if diagonal else 60) * 1024 * 1024),
        cost_estimate=pl.CostEstimate(flops=12_000_000_000 if diagonal else 8_000_000_000, bytes_accessed=12_000_000, transcendentals=26_000_000),
        name="attention_own" if diagonal else "attention_far",
    )(qs, ql, cq, g, c)


def reach(offset):
    return sum((0, 1, 2, 1)[(offset // step) % 4] for step in (1, 4, 16))


offsets = tuple(sorted(range(1, 64), key=lambda offset: -reach(offset)))


def expert_kernel(own_ref, far_ref, own_ml, small_hbm, large_hbm, residual_ref, mix_ref, route_ref, blend_ref, table_ref, weight_ref, gate_hbm, up_hbm, down_hbm, out_ref,
                  gate_w, up_w, down_w, project, part_ref, joined, other, rows, leaving, taken, hidden, made, back, kept, given, swapped,
                  load, pair_send, pair_recv, go_send, go_recv, back_send, back_recv):
    sp, tp = lax.axis_index("sp"), lax.axis_index("tp")
    z, y, x = sp // 16, (sp // 4) % 4, sp % 4

    def chip(offset, sign):
        oz, oy, ox = offset // 16, (offset // 4) % 4, offset % 4
        return ((z + sign * oz + 4) % 4) * 16 + ((y + sign * oy + 4) % 4) * 4 + (x + sign * ox + 4) % 4

    partner = (sp, 1 - tp)
    loads = [
        pltpu.make_async_copy(source.at[0], target, load.at[k])
        for k, (source, target) in enumerate(((gate_hbm, gate_w), (up_hbm, up_w), (down_hbm, down_w)))
    ]
    heads = pl.ds(pl.multiple_of(tp * 512, 512), 512)
    projections = [
        pltpu.make_async_copy(source.at[heads, :], project.at[pl.ds(512 * k, 512), :], load.at[3 + k])
        for k, source in enumerate((small_hbm, large_hbm))
    ]
    for copy in projections:
        copy.start()
    barrier = pltpu.get_barrier_semaphore()
    for offset in offsets:
        pl.semaphore_signal(barrier, inc=1, device_id=(chip(offset, 1), tp), device_id_type=MESH)
    pl.semaphore_signal(barrier, inc=1, device_id=partner, device_id_type=MESH)
    for copy in loads:
        copy.start()
    far_ml = sum(far_ref[1024 + 32 * k : 1056 + 32 * k, :].astype(f32) for k in range(3))
    for h in range(12):
        size, base = (64, h * 64) if h < 8 else (128, 512 + (h - 8) * 128)
        l_own, l_far = own_ml[16 + h : 17 + h, :], far_ml[16 + h : 17 + h, :]
        m_own = own_ml[h : h + 1, :]
        m_far = jnp.where(l_far > 0, far_ml[h : h + 1, :], far_score)
        most = jnp.maximum(m_own, m_far)
        a, b = l_own * jnp.exp2(m_own - most), l_far * jnp.exp2(m_far - most)
        whole = a + b
        rows_here = slice(base, base + size)
        joined[rows_here, :] = (own_ref[rows_here, :] * (a / whole) + far_ref[rows_here, :].astype(f32) * (b / whole)).astype(bf16)
    attended = joined[...].T
    for copy in projections:
        copy.wait()
    for w in range(0, 2048, 512):
        part_ref[:, w : w + 512] = jnp.dot(attended, project[:, w : w + 512], preferred_element_type=f32).astype(bf16)
    pl.semaphore_wait(barrier, 64)

    def across(source, target, k):
        return pltpu.make_async_remote_copy(
            src_ref=source, dst_ref=target, send_sem=pair_send.at[k], recv_sem=pair_recv.at[k],
            device_id=partner, device_id_type=MESH)

    first = across(part_ref.at[pl.ds((1 - tp) * 128, 128), :], other, 0)
    first.start()
    first.wait()

    def scaled(values, gain):
        return values * lax.rsqrt(jnp.mean(values * values, axis=-1, keepdims=True) + norm_eps) * gain

    mixer = part_ref[pl.ds(pl.multiple_of(tp * 128, 128), 128), :].astype(f32) + other[...].astype(f32)
    mixed = (residual_ref[...].astype(f32) + scaled(mixer, mix_ref[...])).astype(bf16)
    kept[...] = mixed
    given[...] = scaled(mixed.astype(f32), route_ref[...]).astype(bf16)
    mine = pl.ds(pl.multiple_of(tp * 128, 128), 128)
    rows[mine, :] = given[...]
    second = across(given, rows.at[mine, :], 1)
    second.start()
    second.wait_send()
    theirs = rows.at[pl.ds(pl.multiple_of((1 - tp) * 128, 128), 128), :]
    across(theirs, theirs, 1).wait_recv()
    for w in range(0, 2048, 512):
        leaving[:, :, w : w + 512] = jnp.dot(table_ref[...], rows[:, w : w + 512], preferred_element_type=f32).astype(bf16).reshape(64, 8, 512)

    def go(n):
        return pltpu.make_async_remote_copy(
            src_ref=leaving.at[chip(offsets[n], 1)], dst_ref=taken.at[n], send_sem=go_send.at[n], recv_sem=go_recv.at[n],
            device_id=(chip(offsets[n], 1), tp), device_id_type=MESH)

    def come(n):
        return pltpu.make_async_remote_copy(
            src_ref=made.at[n], dst_ref=back.at[sp], send_sem=back_send.at[n], recv_sem=back_recv.at[n],
            device_id=(chip(offsets[n], -1), tp), device_id_type=MESH)

    def came(n):
        ref = back.at[chip(offsets[n], 1)]
        return pltpu.make_async_remote_copy(
            src_ref=ref, dst_ref=ref, send_sem=back_send.at[n], recv_sem=back_recv.at[n], device_id=partner, device_id_type=MESH)

    for n in range(63):
        go(n).start()
    taken[63] = leaving[sp]
    for copy in loads:
        copy.wait()
    for group in (0, 1):
        members = range(32 * group, min(32 * group + 32, 63))
        for n in members:
            go(n).wait_recv()
        arrivals = taken[32 * group : 32 * group + 32].reshape(256, 2048)

        def widen(k, _):
            w = pl.ds(pl.multiple_of(k * 256, 256), 256)
            gated = jnp.dot(arrivals, gate_w[:, w], preferred_element_type=f32)
            upped = jnp.dot(arrivals, up_w[:, w], preferred_element_type=f32)
            hidden[:, w] = (gated / (1.0 + jnp.exp(-gated)) * upped).astype(bf16)
            return 0

        lax.fori_loop(0, 4, widen, 0)

        def narrow(k, _):
            w = pl.ds(pl.multiple_of(k * 512, 512), 512)
            made[32 * group : 32 * group + 32, :, w] = jnp.dot(hidden[...], down_w[:, w], preferred_element_type=f32).astype(bf16).reshape(32, 8, 512)
            return 0

        lax.fori_loop(0, 4, narrow, 0)
        for n in members:
            come(n).start()
    back[sp] = made[63]
    for n in range(63):
        go(n).wait_send()
    for n in range(63):
        came(n).wait_recv()
    for n in range(63):
        come(n).wait_send()
    ours = pl.ds(pl.multiple_of(tp * 128, 128), 128)
    away = pl.ds(pl.multiple_of((1 - tp) * 128, 128), 128)

    for w in range(0, 2048, 512):
        returned = back[:, :, w : w + 512].reshape(512, 512)
        given[:, w : w + 512] = (
            jnp.dot(weight_ref[away, 0:512], returned, preferred_element_type=f32)
            + jnp.dot(weight_ref[away, 512:1024], returned, preferred_element_type=f32)
        ).astype(bf16)
    third = across(given, swapped, 2)
    third.start()
    parts = []
    for w in range(0, 2048, 512):
        returned = back[:, :, w : w + 512].reshape(512, 512)
        parts.append(
            jnp.dot(weight_ref[ours, 0:512], returned, preferred_element_type=f32)
            + jnp.dot(weight_ref[ours, 512:1024], returned, preferred_element_type=f32)
        )
    third.wait()
    blended = jnp.concatenate(parts, axis=1) + swapped[...].astype(f32)
    out_ref[...] = (kept[...].astype(f32) + scaled(blended, blend_ref[...])).astype(bf16)


def experts(own_o, far_o, own_ml, out_small, out_large, residual, gain_mix, gain_route, gain_blend, table, weight, w_gate, w_up, w_down):
    V = pl.BlockSpec(memory_space=pltpu.VMEM)
    A = pl.BlockSpec(memory_space=pl.ANY)
    VM, DMA = pltpu.VMEM, pltpu.SemaphoreType.DMA
    return pl.pallas_call(
        expert_kernel,
        out_shape=jax.ShapeDtypeStruct((128, 2048), bf16),
        in_specs=[V] * 3 + [A] * 2 + [V] * 6 + [A] * 3,
        out_specs=V,
        scratch_shapes=[
            VM((2048, 1024), bf16), VM((2048, 1024), bf16), VM((1024, 2048), bf16),
            VM((1024, 2048), bf16), VM((256, 2048), bf16), VM((1024, 256), bf16),
            VM((128, 2048), bf16), VM((256, 2048), bf16), VM((64, 8, 2048), bf16), VM((64, 8, 2048), bf16),
            VM((256, 1024), bf16), VM((64, 8, 2048), bf16), VM((64, 8, 2048), bf16),
            VM((128, 2048), bf16), VM((128, 2048), bf16), VM((128, 2048), bf16),
            DMA((5,)), DMA((3,)), DMA((3,)), DMA((64,)), DMA((64,)), DMA((64,)), DMA((64,)),
        ],
        compiler_params=pltpu.CompilerParams(collective_id=1, has_side_effects=True, vmem_limit_bytes=50 * 1024 * 1024),
        name="experts",
    )(own_o, far_o, own_ml, out_small, out_large, residual, gain_mix, gain_route, gain_blend, table, weight, w_gate, w_up, w_down)


def on_device(
    queries_small,
    queries_large,
    kv_small,
    kv_large,
    cum_small,
    cum_large,
    residual,
    out_small,
    out_large,
    gain_mix,
    gain_route,
    gain_blend,
    w_gate,
    w_up,
    w_down,
    route,
    route_bias,
):
    chips = lax.axis_size("sp")
    to_late = [(i, chips - 1 - i) for i in range(chips // 2)]
    g, c, *far_q, table, weight, gates = gather(kv_small, kv_large, cum_small, cum_large, queries_small, queries_large, route, route_bias[None])
    g, c = g.reshape(chips * 256, 384), c.reshape(chips, 32, 128)
    far_o = attention(*far_q, g, c, False)
    far_o = lax.ppermute(far_o, "sp", to_late)
    own_o, own_ml = attention(queries_small, queries_large, gates, g, c, True)
    return experts(
        own_o, far_o, own_ml, out_small, out_large,
        residual, gain_mix[None], gain_route[None], gain_blend[None], table, weight, w_gate, w_up, w_down
    )


def solution(mesh):
    in_specs = (
        P("sp", "tp"),
        P("sp", "tp"),
        P("sp", None),
        P("sp", None),
        P("tp", "sp"),
        P("tp", "sp"),
        P(("sp", "tp"), None),
        P(),
        P(),
        P(),
        P(),
        P(),
        P(("sp", "tp"), None, None),
        P(("sp", "tp"), None, None),
        P(("sp", "tp"), None, None),
        P(None, ("sp", "tp")),
        P(("sp", "tp")),
    )
    out_specs = P(("sp", "tp"), None)
    return jax.shard_map(
        on_device, mesh=mesh, in_specs=in_specs, out_specs=out_specs, check_vma=False
    )
```
